32 devices in a mesh: gr: 2 (over y), sp: 4 (over z), tp: 4 (over x, core).
Axes of the slice: x: 2, y: 2, z: 4, core: 2. Of those that a mesh axis runs over, the one named last changes fastest.
Arguments:
- tokens: bfloat16 [8, 8192, 2048], P(('gr', 'tp'), 'sp'), may hold values from -6 to 6
- kv_weight: bfloat16 [2048, 1024], replicated, may hold values from -0.125 to 0.125
- queries: bfloat16 [8, 1536], P(('gr', 'tp')), may hold values from -6 to 6
- score_offset: float32 [24], replicated, may hold values from -10.5 to -3.5
Outputs:
- cache: bfloat16 [8, 4, 8192, 256], P(('gr', 'tp'), 'sp')
- read: bfloat16 [8, 1536], P(('gr', 'tp'))
The draws below stay inside these ranges and needn't reach their ends.
All inputs are finite; a program needn't handle non-finite values.
Results may differ from the reference program's by a relative error of at most 0.0085.
Values may be sent and summed in bfloat16 or wider, within the bound.
A program may use at most 64 MiB of HBM per device.

```python
import jax
import jax.numpy as jnp
from jax import lax

D = 2048
H = 24
KVH = 8
HD = 64
LEN = 8192
KVF = 1024
CB = 4
W = 256
SEQ_DEV = 1
GROUPS = 8
SEQS = 8
N_SP = 4


def levels(own_key, dims, pieces, low, top_value):
    def one(dim, parts):
        draws = jax.random.uniform(jax.random.fold_in(jax.random.fold_in(own_key, 6), dim), (parts,), jnp.float32, low / len(pieces), top_value / len(pieces))
        return jnp.repeat(jnp.exp(draws), dims[dim] // parts).reshape((-1,) + (1,) * (len(dims) - dim - 1))

    loudness = one(*pieces[0])
    for cut in pieces[1:]:
        loudness = loudness * one(*cut)
    return loudness


def bell_draw(own_key, dims, scale, reach, pieces=(), dtype=jnp.bfloat16):
    entries = scale * jax.random.normal(own_key, dims, jnp.float32)
    if pieces:
        entries = entries * levels(own_key, dims, pieces, -0.22, 0.18)
    return jnp.clip(entries, -reach, reach).astype(dtype)


def setup_inputs(seed: int = 0) -> dict:
    key_list = jax.random.split(jax.random.key(seed), 5)
    tokens = bell_draw(key_list[0], (SEQS, LEN, D), 1.0, 6.0, ((0, 8), (1, 4)))
    kv_weight = bell_draw(key_list[1], (D, KVF), D ** -0.5, 0.125)
    queries = bell_draw(key_list[2], (SEQS, H * HD), 1.0, 6.0, ((0, 8),))
    score_offset = jnp.clip(jax.random.uniform(key_list[3], (H,), jnp.float32, -10.5, -3.5), -10.5, -3.5)
    return dict(tokens=tokens, kv_weight=kv_weight, queries=queries, score_offset=score_offset)


def reference(tokens, kv_weight, queries, score_offset):
    projected = jnp.dot(tokens.reshape(SEQS * LEN, D), kv_weight, preferred_element_type=jnp.float32).astype(jnp.bfloat16)
    projected = projected.reshape(SEQS, LEN, KVF)
    cache = projected.reshape(GROUPS, SEQ_DEV, LEN, CB, W).transpose(0, 1, 3, 2, 4).reshape(GROUPS, N_SP, LEN, W)
    pairs = projected.reshape(SEQS, LEN, 2, KVH, HD)
    offsets = score_offset.reshape(KVH, H // KVH)

    def one_sequence(args):
        query_row, pair_rows = args
        query_heads = query_row.astype(jnp.float32).reshape(KVH, H // KVH, HD)
        key_rows = pair_rows[:, 0].astype(jnp.float32)
        value_rows = pair_rows[:, 1].astype(jnp.float32)
        logits = jnp.einsum('ngd,pnd->ngp', query_heads, key_rows) * (HD ** -0.5) + offsets[:, :, None]
        keep_log = jax.nn.log_sigmoid(-logits)
        between = lax.cumsum(keep_log, axis=2, reverse=True) - keep_log
        weights = jnp.exp(jax.nn.log_sigmoid(logits) + between)
        return jnp.einsum('ngp,pnd->ngd', weights, value_rows).reshape(H * HD)

    read = lax.map(one_sequence, (queries, pairs)).astype(jnp.bfloat16)
    return cache, read
```

```python
import functools

import jax
import jax.numpy as jnp
from jax import lax
from jax.experimental import pallas as pl
from jax.experimental.pallas import tpu as pltpu
from jax.sharding import PartitionSpec as P

KVH = 8
HD = 64


def prefix(shard, axis, combine, identity):
    size, index = (lax.axis_size(axis), lax.axis_index(axis))
    everything = lax.all_gather(shard, axis)
    start = jnp.broadcast_to(jnp.asarray(identity, shard.dtype), shard.shape)

    def hop(k, before):
        at = size - 1 - k
        reached = at > index
        new = combine(before, everything[at])
        return jnp.where(reached, new, before)

    return lax.fori_loop(0, size, hop, start)


def add_terms(earlier, later):
    return earlier + later


def finish(contribution):
    return lax.psum(contribution, "sp").astype(jnp.bfloat16)


def local_plain(tokens, kv_weight, queries, score_offset):
    seq_count, pos_rows, model_width = tokens.shape
    features = kv_weight.shape[1]
    slot_count = lax.axis_size("sp")
    blocks = slot_count // seq_count
    block_width = features // blocks
    half_blocks = blocks // 2
    heads = score_offset.shape[0]
    group_size = heads // KVH
    per_block = block_width // HD
    projected = jnp.einsum(
        "spd,dcw->scpw",
        tokens,
        kv_weight.reshape(model_width, blocks, block_width),
        preferred_element_type=jnp.float32,
    ).astype(jnp.bfloat16)
    received = lax.all_to_all(
        projected.reshape(slot_count, pos_rows, block_width),
        "sp",
        split_axis=0,
        concat_axis=1,
        tiled=True,
    )
    length = received.shape[1]
    cache = received.reshape(1, 1, length, block_width)
    key_part = projected[:, :half_blocks].reshape(seq_count, half_blocks, pos_rows, per_block, HD)
    value_part = (
        projected[:, half_blocks:]
        .reshape(seq_count, half_blocks, pos_rows, per_block, HD)
        .astype(jnp.float32)
    )
    query_heads = queries.reshape(seq_count, half_blocks, per_block, group_size, HD)
    offsets = score_offset.reshape(half_blocks, per_block, group_size)
    logits = jnp.einsum(
        "scvgd,scpvd->scvgp", query_heads, key_part, preferred_element_type=jnp.float32
    )
    logits = logits * HD ** (-0.5) + offsets[None, :, :, :, None]
    keep_log = jax.nn.log_sigmoid(-logits)
    between = lax.cumsum(keep_log, axis=4, reverse=True) - keep_log
    totals = jnp.sum(keep_log, axis=4)
    later_keep = prefix(totals, "sp", add_terms, jnp.zeros_like(totals))
    weights = jnp.exp(jax.nn.log_sigmoid(logits) + between + later_keep[..., None])
    weighted = jnp.einsum("scvgp,scpvd->scvgd", weights, value_part)
    contribution = weighted.reshape(seq_count, heads * HD)
    return (cache, finish(contribution))


CHUNK = 256
LANES = 128
MESH = pl.DeviceIdType.MESH


def exchange_kernel(
    count,
    tok_hbm,
    w_hbm,
    q_ref,
    off_ref,
    recv,
    read_ref,
    tok,
    wts,
    proj,
    qbig,
    part,
    parts,
    tok_sem,
    w_sem,
    send_sem,
    recv_sem,
    psend_sem,
    precv_sem,
):
    me = lax.axis_index("sp")
    rows = tok.shape[0]
    width = wts.shape[2]
    chunks = rows // CHUNK
    heads = q_ref.shape[0]
    group = heads // KVH
    half = count // 2

    def dest(j):
        return lax.rem(me + 1 + j, count)

    def tok_copy(c):
        at = pl.ds(pl.multiple_of(c * CHUNK, CHUNK), CHUNK)
        return pltpu.make_async_copy(tok_hbm.at[at, :], tok.at[at, :], tok_sem.at[c])

    def w_copy(d):
        at = pl.ds(pl.multiple_of(d * width, width), width)
        return pltpu.make_async_copy(w_hbm.at[:, at], wts.at[d], w_sem.at[d])

    tok_copy(chunks - 1).start()
    for j in range(count):
        w_copy(dest(j)).start()

    @pl.loop(1, chunks)
    def _(i):
        tok_copy(chunks - 1 - i).start()

    barrier = pltpu.get_barrier_semaphore()
    for j in range(count - 1):
        pl.semaphore_signal(barrier, inc=1, device_id={"sp": dest(j)}, device_id_type=MESH)

    spread = jnp.concatenate([q_ref[...].astype(jnp.float32)] * KVH, axis=1)
    column = lax.broadcasted_iota(jnp.int32, spread.shape, 1) // HD
    row = lax.broadcasted_iota(jnp.int32, spread.shape, 0) // group
    mine = column == row
    qbig[...] = jnp.where(mine, spread, 0.0).astype(jnp.bfloat16)
    earlier = lax.broadcasted_iota(jnp.int32, (CHUNK, CHUNK), 1)
    later = lax.broadcasted_iota(jnp.int32, (CHUNK, CHUNK), 0)
    after = jnp.where(later > earlier, 1.0, 0.0).astype(jnp.bfloat16)

    pl.semaphore_wait(barrier, count - 1)

    interior = jnp.logical_and(me > 0, me < count - 1)

    def adjacent(d):
        return jnp.logical_or(d == me + 1, d == me - 1)

    def block_copy(d, c):
        here = pl.ds(pl.multiple_of(c * CHUNK, CHUNK), CHUNK)
        there = pl.ds(pl.multiple_of(me * rows + c * CHUNK, CHUNK), CHUNK)
        return pltpu.make_async_remote_copy(
            src_ref=proj.at[d, here, :],
            dst_ref=recv.at[there, :],
            send_sem=send_sem.at[d],
            recv_sem=recv_sem.at[me],
            device_id={"sp": d},
            device_id_type=MESH,
        )

    def step(i, state):
        kept, total = state
        c = chunks - 1 - i
        at = pl.ds(pl.multiple_of(c * CHUNK, CHUNK), CHUNK)
        tok_copy(c).wait()
        for j in range(count):
            d = dest(j)

            @pl.when(i == 0)
            def _():
                w_copy(d).wait()

            block = jnp.dot(
                tok[at, :], wts[d], preferred_element_type=jnp.float32
            ).astype(jnp.bfloat16)
            proj[d, at, :] = block
            if j == count - 1:
                own = pl.ds(pl.multiple_of(me * rows + c * CHUNK, CHUNK), CHUNK)
                recv[own, :] = block
            if j > 0:
                before = dest(j - 1)

                @pl.when(jnp.logical_or(interior, adjacent(before)))
                def _():
                    block_copy(before, c).start()

        logits = jnp.zeros((heads, CHUNK), jnp.float32)
        for b in range(half):
            logits = logits + lax.dot_general(
                qbig[:, b * width : (b + 1) * width],
                proj[b, at, :],
                (((1,), (1,)), ((), ())),
                preferred_element_type=jnp.float32,
            )
        logits = logits * HD ** (-0.5) + off_ref[...]
        keep = -(jnp.maximum(logits, 0.0) + jnp.log1p(jnp.exp(-jnp.abs(logits))))
        high = keep.astype(jnp.bfloat16)
        rest = keep - high.astype(jnp.float32)
        mid = rest.astype(jnp.bfloat16)
        low = (rest - mid.astype(jnp.float32)).astype(jnp.bfloat16)
        sums = jnp.dot(
            jnp.concatenate([high, mid, low], axis=0), after, preferred_element_type=jnp.float32
        )
        between = sums[:heads] + sums[heads : 2 * heads] + sums[2 * heads :]
        weight = jnp.exp(logits + keep + between + kept)
        weight_high = weight.astype(jnp.bfloat16)
        weight_low = (weight - weight_high.astype(jnp.float32)).astype(jnp.bfloat16)
        both = jnp.concatenate([weight_high, weight_low], axis=0)
        summed = jnp.concatenate(
            [
                jnp.dot(both, proj[half + b, at, :], preferred_element_type=jnp.float32)
                for b in range(half)
            ],
            axis=1,
        )
        total = total + summed[:heads] + summed[heads:]
        kept = kept + jnp.sum(keep, axis=1, keepdims=True)
        return kept, total

    kept, total = lax.fori_loop(
        0,
        chunks,
        step,
        (jnp.zeros((heads, 1), jnp.float32), jnp.zeros((heads, KVH * HD), jnp.float32)),
    )
    total = jnp.where(mine, total, 0.0)
    folded = total[:, :LANES]
    for g in range(1, KVH * HD // LANES):
        folded = folded + total[:, g * LANES : (g + 1) * LANES]
    spread_kept = jnp.broadcast_to(kept, (heads, LANES))
    part[0] = folded
    part[1] = spread_kept
    parts[me, 0] = folded
    parts[me, 1] = spread_kept

    @pl.when(jnp.logical_not(interior))
    def _():
        @pl.loop(0, 1)
        def _(i):
            for j in range(count - 1):
                d = dest(j)

                @pl.when(jnp.logical_not(adjacent(d)))
                def _():
                    block_copy(d, chunks - 1 - i).start()

    def part_copy(d):
        return pltpu.make_async_remote_copy(
            src_ref=part,
            dst_ref=parts.at[me],
            send_sem=psend_sem.at[d],
            recv_sem=precv_sem.at[me],
            device_id={"sp": d},
            device_id_type=MESH,
        )

    for j in range(count - 1):
        part_copy(dest(j)).start()

    @pl.when(jnp.logical_not(interior))
    def _():
        @pl.loop(1, chunks)
        def _(i):
            for j in range(count - 1):
                d = dest(j)

                @pl.when(jnp.logical_not(adjacent(d)))
                def _():
                    block_copy(d, chunks - 1 - i).start()

    for j in range(count - 1):
        d = dest(j)
        pltpu.make_async_remote_copy(
            src_ref=part,
            dst_ref=parts.at[d],
            send_sem=psend_sem.at[d],
            recv_sem=precv_sem.at[d],
            device_id={"sp": d},
            device_id_type=MESH,
        ).wait()
    left = jnp.zeros((heads, LANES), jnp.float32)
    out = jnp.zeros((heads, LANES), jnp.float32)
    for z in range(count - 1, -1, -1):
        out = out + jnp.exp(left) * parts[z, 0]
        left = left + parts[z, 1]
    turned = pltpu.roll(out, HD, axis=1)
    low_half = lax.broadcasted_iota(jnp.int32, (1, LANES), 1) < HD
    for m in range(heads // 2):
        first, second = 2 * m, 2 * m + 1
        from_first = out if (first // group) % 2 == 0 else turned
        from_second = out if (second // group) % 2 == 1 else turned
        piece = jnp.where(
            low_half, from_first[first : first + 1], from_second[second : second + 1]
        )
        read_ref[:, m * LANES : (m + 1) * LANES] = piece.astype(read_ref.dtype)
    for j in range(count - 1):
        d = dest(j)
        pltpu.make_async_remote_copy(
            src_ref=proj.at[d],
            dst_ref=recv.at[pl.ds(pl.multiple_of(d * rows, CHUNK), rows), :],
            send_sem=send_sem.at[d],
            recv_sem=recv_sem.at[d],
            device_id={"sp": d},
            device_id_type=MESH,
        ).wait()


def place_kernel(count, got, read, cache, read_out, sems):
    rows = got.shape[0] // count
    copies = []
    for k in range(count):
        at = pl.ds(k * rows, rows)
        copies.append(pltpu.make_async_copy(got.at[at, :], cache.at[at, :], sems.at[k]))
    copies.append(pltpu.make_async_copy(read, read_out, sems.at[count]))
    for copy in copies:
        copy.start()
    for copy in copies:
        copy.wait()


def local(tokens, kv_weight, queries, score_offset):
    seq_count, rows, model_width = tokens.shape
    features = kv_weight.shape[1]
    heads = score_offset.shape[0]
    count = lax.axis_size("sp")
    width = features // (count // seq_count)
    fits = (
        seq_count == 1
        and count % 2 == 0
        and count > 2
        and width % LANES == 0
        and rows % CHUNK == 0
        and features == 2 * KVH * HD
        and 2 * HD == LANES
        and heads % 2 == 0
    )
    if not fits:
        return local_plain(tokens, kv_weight, queries, score_offset)
    length = rows * count
    vmem = pl.BlockSpec(memory_space=pltpu.VMEM)
    hbm = pl.BlockSpec(memory_space=pltpu.HBM)
    got, read = pl.pallas_call(
        functools.partial(exchange_kernel, count),
        out_shape=(
            pltpu.VMEM((length, width), jnp.bfloat16),
            pltpu.VMEM((1, heads * HD), jnp.bfloat16),
        ),
        in_specs=[hbm, hbm, vmem, vmem],
        out_specs=(vmem, vmem),
        scratch_shapes=[
            pltpu.VMEM((rows, model_width), jnp.bfloat16),
            pltpu.VMEM((count, model_width, width), jnp.bfloat16),
            pltpu.VMEM((count, rows, width), jnp.bfloat16),
            pltpu.VMEM((heads, KVH * HD), jnp.bfloat16),
            pltpu.VMEM((2, heads, LANES), jnp.float32),
            pltpu.VMEM((count, 2, heads, LANES), jnp.float32),
            pltpu.SemaphoreType.DMA((rows // CHUNK,)),
            pltpu.SemaphoreType.DMA((count,)),
            pltpu.SemaphoreType.DMA((count,)),
            pltpu.SemaphoreType.DMA((count,)),
            pltpu.SemaphoreType.DMA((count,)),
            pltpu.SemaphoreType.DMA((count,)),
        ],
        compiler_params=pltpu.CompilerParams(
            collective_id=0, has_side_effects=True, vmem_limit_bytes=44 * 2**20
        ),
    )(
        tokens.reshape(rows, model_width),
        kv_weight,
        queries.reshape(heads, HD),
        score_offset.reshape(heads, 1),
    )
    cache, read = pl.pallas_call(
        functools.partial(place_kernel, count),
        out_shape=(
            jax.ShapeDtypeStruct((length, width), jnp.bfloat16),
            jax.ShapeDtypeStruct((1, heads * HD), jnp.bfloat16),
        ),
        in_specs=[vmem, vmem],
        out_specs=(hbm, hbm),
        scratch_shapes=[pltpu.SemaphoreType.DMA((count + 1,))],
        compiler_params=pltpu.CompilerParams(vmem_limit_bytes=8 * 2**20),
    )(got, read)
    return cache.reshape(1, 1, length, width), read


def solution(mesh):
    placed = (P(("gr", "tp"), "sp", None), P(), P(("gr", "tp"), None), P())
    return jax.shard_map(
        local,
        mesh=mesh,
        in_specs=placed,
        out_specs=(P(("gr", "tp"), "sp", None, None), P(("gr", "tp"), None)),
        check_vma=False,
    )
```

```python
import functools

import jax
import jax.numpy as jnp
from jax import lax
from jax.experimental import pallas as pl
from jax.experimental.pallas import tpu as pltpu
from jax.sharding import PartitionSpec as P

KVH = 8
HD = 64


def prefix(shard, axis, combine, identity):
    size, index = (lax.axis_size(axis), lax.axis_index(axis))
    everything = lax.all_gather(shard, axis)
    start = jnp.broadcast_to(jnp.asarray(identity, shard.dtype), shard.shape)

    def hop(k, before):
        at = size - 1 - k
        reached = at > index
        new = combine(before, everything[at])
        return jnp.where(reached, new, before)

    return lax.fori_loop(0, size, hop, start)


def add_terms(earlier, later):
    return earlier + later


def finish(contribution):
    return lax.psum(contribution, "sp").astype(jnp.bfloat16)


def local_plain(tokens, kv_weight, queries, score_offset):
    seq_count, pos_rows, model_width = tokens.shape
    features = kv_weight.shape[1]
    slot_count = lax.axis_size("sp")
    blocks = slot_count // seq_count
    block_width = features // blocks
    half_blocks = blocks // 2
    heads = score_offset.shape[0]
    group_size = heads // KVH
    per_block = block_width // HD
    projected = jnp.einsum(
        "spd,dcw->scpw",
        tokens,
        kv_weight.reshape(model_width, blocks, block_width),
        preferred_element_type=jnp.float32,
    ).astype(jnp.bfloat16)
    received = lax.all_to_all(
        projected.reshape(slot_count, pos_rows, block_width),
        "sp",
        split_axis=0,
        concat_axis=1,
        tiled=True,
    )
    length = received.shape[1]
    cache = received.reshape(1, 1, length, block_width)
    key_part = projected[:, :half_blocks].reshape(seq_count, half_blocks, pos_rows, per_block, HD)
    value_part = (
        projected[:, half_blocks:]
        .reshape(seq_count, half_blocks, pos_rows, per_block, HD)
        .astype(jnp.float32)
    )
    query_heads = queries.reshape(seq_count, half_blocks, per_block, group_size, HD)
    offsets = score_offset.reshape(half_blocks, per_block, group_size)
    logits = jnp.einsum(
        "scvgd,scpvd->scvgp", query_heads, key_part, preferred_element_type=jnp.float32
    )
    logits = logits * HD ** (-0.5) + offsets[None, :, :, :, None]
    keep_log = jax.nn.log_sigmoid(-logits)
    between = lax.cumsum(keep_log, axis=4, reverse=True) - keep_log
    totals = jnp.sum(keep_log, axis=4)
    later_keep = prefix(totals, "sp", add_terms, jnp.zeros_like(totals))
    weights = jnp.exp(jax.nn.log_sigmoid(logits) + between + later_keep[..., None])
    weighted = jnp.einsum("scvgp,scpvd->scvgd", weights, value_part)
    contribution = weighted.reshape(seq_count, heads * HD)
    return (cache, finish(contribution))


CHUNK = 256
VMEM_LIMIT = 56 * 2**20
LANES = 128
MESH = pl.DeviceIdType.MESH


def exchange_kernel(
    count,
    tok_hbm,
    w_hbm,
    q_ref,
    off_ref,
    recv,
    read_ref,
    tok,
    wts,
    proj,
    qbig,
    part,
    parts,
    tok_sem,
    w_sem,
    send_sem,
    recv_sem,
    psend_sem,
    precv_sem,
):
    me = lax.axis_index("sp")
    rows = tok.shape[0]
    width = wts.shape[2]
    chunks = rows // CHUNK
    heads = off_ref.shape[1]
    group = heads // KVH
    half = count // 2

    way = jnp.where(me < count // 2, 1, -1)

    def dest(j):
        return lax.rem(me + count + way * (1 + j), count)

    def tok_copy(c):
        at = pl.ds(pl.multiple_of(c * CHUNK, CHUNK), CHUNK)
        return pltpu.make_async_copy(tok_hbm.at[at, :], tok.at[at, :], tok_sem.at[c])

    def w_copy(d):
        at = pl.ds(pl.multiple_of(d * width, width), width)
        return pltpu.make_async_copy(w_hbm.at[:, at], wts.at[d], w_sem.at[d])

    tok_copy(chunks - 1).start()
    for j in range(count):
        w_copy(dest(j)).start()

    @pl.loop(1, chunks)
    def _(i):
        tok_copy(chunks - 1 - i).start()

    barrier = pltpu.get_barrier_semaphore()
    for j in range(count - 1):
        pl.semaphore_signal(barrier, inc=1, device_id={"sp": dest(j)}, device_id_type=MESH)

    q_rows = []
    for h in range(heads):
        pair = q_ref[:, h // 2 * LANES : (h // 2 + 1) * LANES].astype(jnp.float32)
        q_rows.append(pair if h % 2 == h // group % 2 else pltpu.roll(pair, HD, axis=1))
    spread = jnp.concatenate(
        [jnp.concatenate(q_rows, axis=0)] * (KVH * HD // LANES), axis=1
    )
    square = (heads, heads)
    diagonal = lax.broadcasted_iota(jnp.int32, square, 0) == lax.broadcasted_iota(
        jnp.int32, square, 1
    )
    offsets = jnp.sum(
        jnp.where(diagonal, jnp.broadcast_to(off_ref[...], square), 0.0), axis=1, keepdims=True
    )
    column = lax.broadcasted_iota(jnp.int32, spread.shape, 1) // HD
    row = lax.broadcasted_iota(jnp.int32, spread.shape, 0) // group
    mine = column == row
    qbig[...] = jnp.where(mine, spread, 0.0).astype(jnp.bfloat16)
    earlier = lax.broadcasted_iota(jnp.int32, (CHUNK, CHUNK), 1)
    later = lax.broadcasted_iota(jnp.int32, (CHUNK, CHUNK), 0)
    after = jnp.where(later > earlier, 1.0, 0.0).astype(jnp.bfloat16)

    interior = jnp.logical_and(me > 0, me < count - 1)

    def adjacent(d):
        return jnp.logical_or(d == me + 1, d == me - 1)

    def block_copy(d, c):
        here = pl.ds(pl.multiple_of(c * CHUNK, CHUNK), CHUNK)
        there = pl.ds(pl.multiple_of(me * rows + c * CHUNK, CHUNK), CHUNK)
        return pltpu.make_async_remote_copy(
            src_ref=proj.at[d, here, :],
            dst_ref=recv.at[there, :],
            send_sem=send_sem.at[d],
            recv_sem=recv_sem.at[me],
            device_id={"sp": d},
            device_id_type=MESH,
        )

    def step(i, state):
        kept, total = state
        c = chunks - 1 - i
        at = pl.ds(pl.multiple_of(c * CHUNK, CHUNK), CHUNK)
        tok_copy(c).wait()
        for j in range(count):
            d = dest(j)

            @pl.when(i == 0)
            def _():
                w_copy(d).wait()

            block = jnp.dot(
                tok[at, :], wts[d], preferred_element_type=jnp.float32
            ).astype(jnp.bfloat16)
            proj[d, at, :] = block
            if j == count - 1:
                own = pl.ds(pl.multiple_of(me * rows + c * CHUNK, CHUNK), CHUNK)
                recv[own, :] = block
            if j > 0:
                before = dest(j - 1)
                if j == 1:

                    @pl.when(i == 0)
                    def _():
                        pl.semaphore_wait(barrier, count - 1)

                @pl.when(jnp.logical_or(interior, adjacent(before)))
                def _():
                    block_copy(before, c).start()

        logits = jnp.zeros((heads, CHUNK), jnp.float32)
        for b in range(half):
            logits = logits + lax.dot_general(
                qbig[:, b * width : (b + 1) * width],
                proj[b, at, :],
                (((1,), (1,)), ((), ())),
                preferred_element_type=jnp.float32,
            )
        logits = logits * HD ** (-0.5) + offsets
        keep = -(jnp.maximum(logits, 0.0) + jnp.log1p(jnp.exp(-jnp.abs(logits))))
        high = keep.astype(jnp.bfloat16)
        rest = keep - high.astype(jnp.float32)
        mid = rest.astype(jnp.bfloat16)
        low = (rest - mid.astype(jnp.float32)).astype(jnp.bfloat16)
        sums = jnp.dot(
            jnp.concatenate([high, mid, low], axis=0), after, preferred_element_type=jnp.float32
        )
        between = sums[:heads] + sums[heads : 2 * heads] + sums[2 * heads :]
        weight = jnp.exp(logits + keep + between + kept)
        weight_high = weight.astype(jnp.bfloat16)
        weight_low = (weight - weight_high.astype(jnp.float32)).astype(jnp.bfloat16)
        both = jnp.concatenate([weight_high, weight_low], axis=0)
        summed = jnp.concatenate(
            [
                jnp.dot(both, proj[half + b, at, :], preferred_element_type=jnp.float32)
                for b in range(half)
            ],
            axis=1,
        )
        total = total + summed[:heads] + summed[heads:]
        kept = kept + jnp.sum(keep, axis=1, keepdims=True)
        return kept, total

    kept, total = lax.fori_loop(
        0,
        chunks,
        step,
        (jnp.zeros((heads, 1), jnp.float32), jnp.zeros((heads, KVH * HD), jnp.float32)),
    )
    total = jnp.where(mine, total, 0.0)
    folded = total[:, :LANES]
    for g in range(1, KVH * HD // LANES):
        folded = folded + total[:, g * LANES : (g + 1) * LANES]
    spread_kept = jnp.broadcast_to(kept, (heads, LANES))
    part[0] = folded
    part[1] = spread_kept
    parts[me, 0] = folded
    parts[me, 1] = spread_kept

    @pl.when(jnp.logical_not(interior))
    def _():
        @pl.loop(0, 1)
        def _(i):
            for j in range(count - 1):
                d = dest(j)

                @pl.when(jnp.logical_not(adjacent(d)))
                def _():
                    block_copy(d, chunks - 1 - i).start()

    def part_copy(d):
        return pltpu.make_async_remote_copy(
            src_ref=part,
            dst_ref=parts.at[me],
            send_sem=psend_sem.at[d],
            recv_sem=precv_sem.at[me],
            device_id={"sp": d},
            device_id_type=MESH,
        )

    for j in range(count - 1):
        part_copy(dest(j)).start()

    @pl.when(jnp.logical_not(interior))
    def _():
        @pl.loop(1, chunks)
        def _(i):
            for j in range(count - 1):
                d = dest(j)

                @pl.when(jnp.logical_not(adjacent(d)))
                def _():
                    block_copy(d, chunks - 1 - i).start()

    for j in range(count - 1):
        d = dest(j)
        pltpu.make_async_remote_copy(
            src_ref=part,
            dst_ref=parts.at[d],
            send_sem=psend_sem.at[d],
            recv_sem=precv_sem.at[d],
            device_id={"sp": d},
            device_id_type=MESH,
        ).wait()
    left = jnp.zeros((heads, LANES), jnp.float32)
    out = jnp.zeros((heads, LANES), jnp.float32)
    for z in range(count - 1, -1, -1):
        out = out + jnp.exp(left) * parts[z, 0]
        left = left + parts[z, 1]
    turned = pltpu.roll(out, HD, axis=1)
    low_half = lax.broadcasted_iota(jnp.int32, (1, LANES), 1) < HD
    for m in range(heads // 2):
        first, second = 2 * m, 2 * m + 1
        from_first = out if (first // group) % 2 == 0 else turned
        from_second = out if (second // group) % 2 == 1 else turned
        piece = jnp.where(
            low_half, from_first[first : first + 1], from_second[second : second + 1]
        )
        read_ref[:, m * LANES : (m + 1) * LANES] = piece.astype(read_ref.dtype)
    for j in range(count - 1):
        d = dest(j)
        pltpu.make_async_remote_copy(
            src_ref=proj.at[d],
            dst_ref=recv.at[pl.ds(pl.multiple_of(d * rows, CHUNK), rows), :],
            send_sem=send_sem.at[d],
            recv_sem=recv_sem.at[d],
            device_id={"sp": d},
            device_id_type=MESH,
        ).wait()


def place_kernel(count, got, read, cache, read_out, sems):
    rows = got.shape[0] // count
    copies = []
    for k in range(count):
        at = pl.ds(k * rows, rows)
        copies.append(pltpu.make_async_copy(got.at[at, :], cache.at[at, :], sems.at[k]))
    copies.append(pltpu.make_async_copy(read, read_out, sems.at[count]))
    for copy in copies:
        copy.start()
    for copy in copies:
        copy.wait()


def local(tokens, kv_weight, queries, score_offset):
    seq_count, rows, model_width = tokens.shape
    features = kv_weight.shape[1]
    heads = score_offset.shape[0]
    count = lax.axis_size("sp")
    width = features // (count // seq_count)
    fits = (
        seq_count == 1
        and count % 2 == 0
        and count > 2
        and width % LANES == 0
        and rows % CHUNK == 0
        and features == 2 * KVH * HD
        and 2 * HD == LANES
        and heads % 2 == 0
    )
    if not fits:
        return local_plain(tokens, kv_weight, queries, score_offset)
    length = rows * count
    vmem = pl.BlockSpec(memory_space=pltpu.VMEM)
    hbm = pl.BlockSpec(memory_space=pltpu.HBM)
    got, read = pl.pallas_call(
        functools.partial(exchange_kernel, count),
        out_shape=(
            pltpu.VMEM((length, width), jnp.bfloat16),
            pltpu.VMEM((1, heads * HD), jnp.bfloat16),
        ),
        in_specs=[hbm, hbm, vmem, vmem],
        out_specs=(vmem, vmem),
        scratch_shapes=[
            pltpu.VMEM((rows, model_width), jnp.bfloat16),
            pltpu.VMEM((count, model_width, width), jnp.bfloat16),
            pltpu.VMEM((count, rows, width), jnp.bfloat16),
            pltpu.VMEM((heads, KVH * HD), jnp.bfloat16),
            pltpu.VMEM((2, heads, LANES), jnp.float32),
            pltpu.VMEM((count, 2, heads, LANES), jnp.float32),
            pltpu.SemaphoreType.DMA((rows // CHUNK,)),
            pltpu.SemaphoreType.DMA((count,)),
            pltpu.SemaphoreType.DMA((count,)),
            pltpu.SemaphoreType.DMA((count,)),
            pltpu.SemaphoreType.DMA((count,)),
            pltpu.SemaphoreType.DMA((count,)),
        ],
        compiler_params=pltpu.CompilerParams(
            collective_id=0, has_side_effects=True, vmem_limit_bytes=VMEM_LIMIT
        ),
    )(
        tokens.reshape(rows, model_width),
        kv_weight,
        queries,
        score_offset.reshape(1, heads),
    )
    cache, read = pl.pallas_call(
        functools.partial(place_kernel, count),
        out_shape=(
            jax.ShapeDtypeStruct((length, width), jnp.bfloat16),
            jax.ShapeDtypeStruct((1, heads * HD), jnp.bfloat16),
        ),
        in_specs=[vmem, vmem],
        out_specs=(hbm, hbm),
        scratch_shapes=[pltpu.SemaphoreType.DMA((count + 1,))],
        compiler_params=pltpu.CompilerParams(vmem_limit_bytes=8 * 2**20),
    )(got, read)
    return cache.reshape(1, 1, length, width), read


def solution(mesh):
    placed = (P(("gr", "tp"), "sp", None), P(), P(("gr", "tp"), None), P())
    return jax.shard_map(
        local,
        mesh=mesh,
        in_specs=placed,
        out_specs=(P(("gr", "tp"), "sp", None, None), P(("gr", "tp"), None)),
        check_vma=False,
    )
```

```python
import functools

import jax
import jax.numpy as jnp
from jax import lax
from jax.experimental import pallas as pl
from jax.experimental.pallas import tpu as pltpu
from jax.sharding import PartitionSpec as P

KVH = 8
HD = 64


def prefix(shard, axis, combine, identity):
    size, index = (lax.axis_size(axis), lax.axis_index(axis))
    everything = lax.all_gather(shard, axis)
    start = jnp.broadcast_to(jnp.asarray(identity, shard.dtype), shard.shape)

    def hop(k, before):
        at = size - 1 - k
        reached = at > index
        new = combine(before, everything[at])
        return jnp.where(reached, new, before)

    return lax.fori_loop(0, size, hop, start)


def add_terms(earlier, later):
    return earlier + later


def finish(contribution):
    return lax.psum(contribution, "sp").astype(jnp.bfloat16)


def local_plain(tokens, kv_weight, queries, score_offset):
    seq_count, pos_rows, model_width = tokens.shape
    features = kv_weight.shape[1]
    slot_count = lax.axis_size("sp")
    blocks = slot_count // seq_count
    block_width = features // blocks
    half_blocks = blocks // 2
    heads = score_offset.shape[0]
    group_size = heads // KVH
    per_block = block_width // HD
    projected = jnp.einsum(
        "spd,dcw->scpw",
        tokens,
        kv_weight.reshape(model_width, blocks, block_width),
        preferred_element_type=jnp.float32,
    ).astype(jnp.bfloat16)
    received = lax.all_to_all(
        projected.reshape(slot_count, pos_rows, block_width),
        "sp",
        split_axis=0,
        concat_axis=1,
        tiled=True,
    )
    length = received.shape[1]
    cache = received.reshape(1, 1, length, block_width)
    key_part = projected[:, :half_blocks].reshape(seq_count, half_blocks, pos_rows, per_block, HD)
    value_part = (
        projected[:, half_blocks:]
        .reshape(seq_count, half_blocks, pos_rows, per_block, HD)
        .astype(jnp.float32)
    )
    query_heads = queries.reshape(seq_count, half_blocks, per_block, group_size, HD)
    offsets = score_offset.reshape(half_blocks, per_block, group_size)
    logits = jnp.einsum(
        "scvgd,scpvd->scvgp", query_heads, key_part, preferred_element_type=jnp.float32
    )
    logits = logits * HD ** (-0.5) + offsets[None, :, :, :, None]
    keep_log = jax.nn.log_sigmoid(-logits)
    between = lax.cumsum(keep_log, axis=4, reverse=True) - keep_log
    totals = jnp.sum(keep_log, axis=4)
    later_keep = prefix(totals, "sp", add_terms, jnp.zeros_like(totals))
    weights = jnp.exp(jax.nn.log_sigmoid(logits) + between + later_keep[..., None])
    weighted = jnp.einsum("scvgp,scpvd->scvgd", weights, value_part)
    contribution = weighted.reshape(seq_count, heads * HD)
    return (cache, finish(contribution))


CHUNK = 128
VMEM_LIMIT = 56 * 2**20
LANES = 128
MESH = pl.DeviceIdType.MESH


def exchange_kernel(
    count,
    tok_hbm,
    w_hbm,
    q_ref,
    off_ref,
    recv,
    read_ref,
    tok,
    wts,
    proj,
    qbig,
    part,
    parts,
    tok_sem,
    w_sem,
    send_sem,
    recv_sem,
    psend_sem,
    precv_sem,
):
    me = lax.axis_index("sp")
    rows = tok.shape[0]
    width = wts.shape[2]
    chunks = rows // CHUNK
    heads = off_ref.shape[1]
    group = heads // KVH
    half = count // 2

    way = jnp.where(me < count // 2, 1, -1)

    def dest(j):
        return lax.rem(me + count + way * (1 + j), count)

    def tok_copy(c):
        at = pl.ds(pl.multiple_of(c * CHUNK, CHUNK), CHUNK)
        return pltpu.make_async_copy(tok_hbm.at[at, :], tok.at[at, :], tok_sem.at[c])

    def w_copy(d):
        at = pl.ds(pl.multiple_of(d * width, width), width)
        return pltpu.make_async_copy(w_hbm.at[:, at], wts.at[d], w_sem.at[d])

    tok_copy(chunks - 1).start()
    for j in range(2):
        w_copy(dest(j)).start()

    barrier = pltpu.get_barrier_semaphore()
    for j in range(count - 1):
        pl.semaphore_signal(barrier, inc=1, device_id={"sp": dest(j)}, device_id_type=MESH)

    q_rows = []
    for h in range(heads):
        pair = q_ref[:, h // 2 * LANES : (h // 2 + 1) * LANES].astype(jnp.float32)
        q_rows.append(pair if h % 2 == h // group % 2 else pltpu.roll(pair, HD, axis=1))
    spread = jnp.concatenate(
        [jnp.concatenate(q_rows, axis=0)] * (KVH * HD // LANES), axis=1
    )
    square = (heads, heads)
    diagonal = lax.broadcasted_iota(jnp.int32, square, 0) == lax.broadcasted_iota(
        jnp.int32, square, 1
    )
    offsets = jnp.sum(
        jnp.where(diagonal, jnp.broadcast_to(off_ref[...], square), 0.0), axis=1, keepdims=True
    )
    column = lax.broadcasted_iota(jnp.int32, spread.shape, 1) // HD
    row = lax.broadcasted_iota(jnp.int32, spread.shape, 0) // group
    mine = column == row
    qbig[...] = jnp.where(mine, spread, 0.0).astype(jnp.bfloat16)
    earlier = lax.broadcasted_iota(jnp.int32, (CHUNK, CHUNK), 1)
    later = lax.broadcasted_iota(jnp.int32, (CHUNK, CHUNK), 0)
    after = jnp.where(later > earlier, 1.0, 0.0).astype(jnp.bfloat16)

    def deferred(d):
        inner = jnp.logical_and(d > 0, d < count - 1)
        return jnp.logical_and(inner, (d < count // 2) != (me < count // 2))

    def block_copy(d, c):
        here = pl.ds(pl.multiple_of(c * CHUNK, CHUNK), CHUNK)
        there = pl.ds(pl.multiple_of(me * rows + c * CHUNK, CHUNK), CHUNK)
        return pltpu.make_async_remote_copy(
            src_ref=proj.at[d, here, :],
            dst_ref=recv.at[there, :],
            send_sem=send_sem.at[d],
            recv_sem=recv_sem.at[me],
            device_id={"sp": d},
            device_id_type=MESH,
        )

    def step(i, state):
        kept, total = state
        c = chunks - 1 - i
        at = pl.ds(pl.multiple_of(c * CHUNK, CHUNK), CHUNK)
        tok_copy(c).wait()
        for j in range(count):
            d = dest(j)

            @pl.when(i == 0)
            def _():
                w_copy(d).wait()
                if j == 0:
                    for k in range(2, count):
                        w_copy(dest(k)).start()
                    tok_copy(c - 1).start()

            if j == 0:

                @pl.when(i + 2 < chunks)
                def _():
                    tok_copy(c - 2).start()

            block = jnp.dot(
                tok[at, :], wts[d], preferred_element_type=jnp.float32
            ).astype(jnp.bfloat16)
            proj[d, at, :] = block
            if j == count - 1:
                own = pl.ds(pl.multiple_of(me * rows + c * CHUNK, CHUNK), CHUNK)
                recv[own, :] = block
            if j > 0:
                before = dest(j - 1)
                if j == 1:

                    @pl.when(i == 0)
                    def _():
                        pl.semaphore_wait(barrier, count - 1)

                @pl.when(jnp.logical_not(deferred(before)))
                def _():
                    block_copy(before, c).start()

        logits = jnp.zeros((heads, CHUNK), jnp.float32)
        for b in range(half):
            logits = logits + lax.dot_general(
                qbig[:, b * width : (b + 1) * width],
                proj[b, at, :],
                (((1,), (1,)), ((), ())),
                preferred_element_type=jnp.float32,
            )
        logits = logits * HD ** (-0.5) + offsets
        keep = -(jnp.maximum(logits, 0.0) + jnp.log1p(jnp.exp(-jnp.abs(logits))))
        high = keep.astype(jnp.bfloat16)
        rest = keep - high.astype(jnp.float32)
        mid = rest.astype(jnp.bfloat16)
        low = (rest - mid.astype(jnp.float32)).astype(jnp.bfloat16)
        sums = jnp.dot(
            jnp.concatenate([high, mid, low], axis=0), after, preferred_element_type=jnp.float32
        )
        between = sums[:heads] + sums[heads : 2 * heads] + sums[2 * heads :]
        weight = jnp.exp(logits + keep + between + kept)
        weight_high = weight.astype(jnp.bfloat16)
        weight_low = (weight - weight_high.astype(jnp.float32)).astype(jnp.bfloat16)
        both = jnp.concatenate([weight_high, weight_low], axis=0)
        summed = jnp.concatenate(
            [
                jnp.dot(both, proj[half + b, at, :], preferred_element_type=jnp.float32)
                for b in range(half)
            ],
            axis=1,
        )
        total = total + summed[:heads] + summed[heads:]
        kept = kept + jnp.sum(keep, axis=1, keepdims=True)
        return kept, total

    kept, total = lax.fori_loop(
        0,
        chunks,
        step,
        (jnp.zeros((heads, 1), jnp.float32), jnp.zeros((heads, KVH * HD), jnp.float32)),
    )
    total = jnp.where(mine, total, 0.0)
    folded = total[:, :LANES]
    for g in range(1, KVH * HD // LANES):
        folded = folded + total[:, g * LANES : (g + 1) * LANES]
    spread_kept = jnp.broadcast_to(kept, (heads, LANES))
    part[0] = folded
    part[1] = spread_kept
    parts[me, 0] = folded
    parts[me, 1] = spread_kept

    @pl.loop(0, 1)
    def _(i):
        for j in range(count - 1):
            d = dest(j)

            @pl.when(deferred(d))
            def _():
                block_copy(d, chunks - 1 - i).start()

    def part_copy(d):
        return pltpu.make_async_remote_copy(
            src_ref=part,
            dst_ref=parts.at[me],
            send_sem=psend_sem.at[d],
            recv_sem=precv_sem.at[me],
            device_id={"sp": d},
            device_id_type=MESH,
        )

    for j in range(count - 1):
        part_copy(dest(j)).start()

    @pl.loop(1, chunks)
    def _(i):
        for j in range(count - 1):
            d = dest(j)

            @pl.when(deferred(d))
            def _():
                block_copy(d, chunks - 1 - i).start()

    for j in range(count - 1):
        d = dest(j)
        pltpu.make_async_remote_copy(
            src_ref=part,
            dst_ref=parts.at[d],
            send_sem=psend_sem.at[d],
            recv_sem=precv_sem.at[d],
            device_id={"sp": d},
            device_id_type=MESH,
        ).wait()
    left = jnp.zeros((heads, LANES), jnp.float32)
    out = jnp.zeros((heads, LANES), jnp.float32)
    for z in range(count - 1, -1, -1):
        out = out + jnp.exp(left) * parts[z, 0]
        left = left + parts[z, 1]
    turned = pltpu.roll(out, HD, axis=1)
    low_half = lax.broadcasted_iota(jnp.int32, (1, LANES), 1) < HD
    for m in range(heads // 2):
        first, second = 2 * m, 2 * m + 1
        from_first = out if (first // group) % 2 == 0 else turned
        from_second = out if (second // group) % 2 == 1 else turned
        piece = jnp.where(
            low_half, from_first[first : first + 1], from_second[second : second + 1]
        )
        read_ref[:, m * LANES : (m + 1) * LANES] = piece.astype(read_ref.dtype)
    for j in range(count - 1):
        d = dest(j)
        pltpu.make_async_remote_copy(
            src_ref=proj.at[d],
            dst_ref=recv.at[pl.ds(pl.multiple_of(d * rows, CHUNK), rows), :],
            send_sem=send_sem.at[d],
            recv_sem=recv_sem.at[d],
            device_id={"sp": d},
            device_id_type=MESH,
        ).wait()


def place_kernel(count, got, read, cache, read_out, sems):
    rows = got.shape[0] // count
    copies = []
    for k in range(count):
        at = pl.ds(k * rows, rows)
        copies.append(pltpu.make_async_copy(got.at[at, :], cache.at[at, :], sems.at[k]))
    copies.append(pltpu.make_async_copy(read, read_out, sems.at[count]))
    for copy in copies:
        copy.start()
    for copy in copies:
        copy.wait()


def local(tokens, kv_weight, queries, score_offset):
    seq_count, rows, model_width = tokens.shape
    features = kv_weight.shape[1]
    heads = score_offset.shape[0]
    count = lax.axis_size("sp")
    width = features // (count // seq_count)
    fits = (
        seq_count == 1
        and count % 2 == 0
        and count > 2
        and width % LANES == 0
        and rows % CHUNK == 0
        and rows >= 2 * CHUNK
        and features == 2 * KVH * HD
        and 2 * HD == LANES
        and heads % 2 == 0
    )
    if not fits:
        return local_plain(tokens, kv_weight, queries, score_offset)
    length = rows * count
    vmem = pl.BlockSpec(memory_space=pltpu.VMEM)
    hbm = pl.BlockSpec(memory_space=pltpu.HBM)
    got, read = pl.pallas_call(
        functools.partial(exchange_kernel, count),
        out_shape=(
            pltpu.VMEM((length, width), jnp.bfloat16),
            pltpu.VMEM((1, heads * HD), jnp.bfloat16),
        ),
        in_specs=[hbm, hbm, vmem, vmem],
        out_specs=(vmem, vmem),
        scratch_shapes=[
            pltpu.VMEM((rows, model_width), jnp.bfloat16),
            pltpu.VMEM((count, model_width, width), jnp.bfloat16),
            pltpu.VMEM((count, rows, width), jnp.bfloat16),
            pltpu.VMEM((heads, KVH * HD), jnp.bfloat16),
            pltpu.VMEM((2, heads, LANES), jnp.float32),
            pltpu.VMEM((count, 2, heads, LANES), jnp.float32),
            pltpu.SemaphoreType.DMA((rows // CHUNK,)),
            pltpu.SemaphoreType.DMA((count,)),
            pltpu.SemaphoreType.DMA((count,)),
            pltpu.SemaphoreType.DMA((count,)),
            pltpu.SemaphoreType.DMA((count,)),
            pltpu.SemaphoreType.DMA((count,)),
        ],
        compiler_params=pltpu.CompilerParams(
            collective_id=0, has_side_effects=True, vmem_limit_bytes=VMEM_LIMIT
        ),
    )(
        tokens.reshape(rows, model_width),
        kv_weight,
        queries,
        score_offset.reshape(1, heads),
    )
    cache, read = pl.pallas_call(
        functools.partial(place_kernel, count),
        out_shape=(
            jax.ShapeDtypeStruct((length, width), jnp.bfloat16),
            jax.ShapeDtypeStruct((1, heads * HD), jnp.bfloat16),
        ),
        in_specs=[vmem, vmem],
        out_specs=(hbm, hbm),
        scratch_shapes=[pltpu.SemaphoreType.DMA((count + 1,))],
        compiler_params=pltpu.CompilerParams(vmem_limit_bytes=8 * 2**20),
    )(got, read)
    return cache.reshape(1, 1, length, width), read


def solution(mesh):
    placed = (P(("gr", "tp"), "sp", None), P(), P(("gr", "tp"), None), P())
    return jax.shard_map(
        local,
        mesh=mesh,
        in_specs=placed,
        out_specs=(P(("gr", "tp"), "sp", None, None), P(("gr", "tp"), None)),
        check_vma=False,
    )
```

```python
import functools

import jax
import jax.numpy as jnp
from jax import lax
from jax.experimental import pallas as pl
from jax.experimental.pallas import tpu as pltpu
from jax.sharding import PartitionSpec as P

KVH = 8
HD = 64


def prefix(shard, axis, combine, identity):
    size, index = (lax.axis_size(axis), lax.axis_index(axis))
    everything = lax.all_gather(shard, axis)
    start = jnp.broadcast_to(jnp.asarray(identity, shard.dtype), shard.shape)

    def hop(k, before):
        at = size - 1 - k
        reached = at > index
        new = combine(before, everything[at])
        return jnp.where(reached, new, before)

    return lax.fori_loop(0, size, hop, start)


def add_terms(earlier, later):
    return earlier + later


def finish(contribution):
    return lax.psum(contribution, "sp").astype(jnp.bfloat16)


def local_plain(tokens, kv_weight, queries, score_offset):
    seq_count, pos_rows, model_width = tokens.shape
    features = kv_weight.shape[1]
    slot_count = lax.axis_size("sp")
    blocks = slot_count // seq_count
    block_width = features // blocks
    half_blocks = blocks // 2
    heads = score_offset.shape[0]
    group_size = heads // KVH
    per_block = block_width // HD
    projected = jnp.einsum(
        "spd,dcw->scpw",
        tokens,
        kv_weight.reshape(model_width, blocks, block_width),
        preferred_element_type=jnp.float32,
    ).astype(jnp.bfloat16)
    received = lax.all_to_all(
        projected.reshape(slot_count, pos_rows, block_width),
        "sp",
        split_axis=0,
        concat_axis=1,
        tiled=True,
    )
    length = received.shape[1]
    cache = received.reshape(1, 1, length, block_width)
    key_part = projected[:, :half_blocks].reshape(seq_count, half_blocks, pos_rows, per_block, HD)
    value_part = (
        projected[:, half_blocks:]
        .reshape(seq_count, half_blocks, pos_rows, per_block, HD)
        .astype(jnp.float32)
    )
    query_heads = queries.reshape(seq_count, half_blocks, per_block, group_size, HD)
    offsets = score_offset.reshape(half_blocks, per_block, group_size)
    logits = jnp.einsum(
        "scvgd,scpvd->scvgp", query_heads, key_part, preferred_element_type=jnp.float32
    )
    logits = logits * HD ** (-0.5) + offsets[None, :, :, :, None]
    keep_log = jax.nn.log_sigmoid(-logits)
    between = lax.cumsum(keep_log, axis=4, reverse=True) - keep_log
    totals = jnp.sum(keep_log, axis=4)
    later_keep = prefix(totals, "sp", add_terms, jnp.zeros_like(totals))
    weights = jnp.exp(jax.nn.log_sigmoid(logits) + between + later_keep[..., None])
    weighted = jnp.einsum("scvgp,scpvd->scvgd", weights, value_part)
    contribution = weighted.reshape(seq_count, heads * HD)
    return (cache, finish(contribution))


CHUNK = 128
VMEM_LIMIT = 56 * 2**20
LANES = 128
MESH = pl.DeviceIdType.MESH


def exchange_kernel(
    count,
    tok_hbm,
    w_hbm,
    q_ref,
    off_ref,
    recv,
    read_ref,
    tok,
    wts,
    proj,
    qbig,
    part,
    parts,
    tok_sem,
    w_sem,
    send_sem,
    recv_sem,
    psend_sem,
    precv_sem,
):
    me = lax.axis_index("sp")
    rows = tok.shape[0]
    width = wts.shape[2]
    chunks = rows // CHUNK
    heads = off_ref.shape[1]
    group = heads // KVH
    half = count // 2

    lower = me < count // 2

    def dest(j):
        if j == count - 1:
            return me
        down = count - 1 - j
        return jnp.where(
            lower,
            jnp.where(down > me, down, down - 1),
            jnp.where(j < me, j, j + 1),
        )

    def tok_copy(c):
        at = pl.ds(pl.multiple_of(c * CHUNK, CHUNK), CHUNK)
        return pltpu.make_async_copy(tok_hbm.at[at, :], tok.at[at, :], tok_sem.at[c])

    def w_copy(d):
        at = pl.ds(pl.multiple_of(d * width, width), width)
        return pltpu.make_async_copy(w_hbm.at[:, at], wts.at[d], w_sem.at[d])

    barrier = pltpu.get_barrier_semaphore()
    for j in range(count - 1):
        pl.semaphore_signal(barrier, inc=1, device_id={"sp": dest(j)}, device_id_type=MESH)

    tok_copy(chunks - 1).start()
    for j in range(2):
        w_copy(dest(j)).start()

    q_rows = []
    for h in range(heads):
        pair = q_ref[:, h // 2 * LANES : (h // 2 + 1) * LANES].astype(jnp.float32)
        q_rows.append(pair if h % 2 == h // group % 2 else pltpu.roll(pair, HD, axis=1))
    spread = jnp.concatenate(
        [jnp.concatenate(q_rows, axis=0)] * (KVH * HD // LANES), axis=1
    )
    square = (heads, heads)
    diagonal = lax.broadcasted_iota(jnp.int32, square, 0) == lax.broadcasted_iota(
        jnp.int32, square, 1
    )
    offsets = jnp.sum(
        jnp.where(diagonal, jnp.broadcast_to(off_ref[...], square), 0.0), axis=1, keepdims=True
    )
    column = lax.broadcasted_iota(jnp.int32, spread.shape, 1) // HD
    row = lax.broadcasted_iota(jnp.int32, spread.shape, 0) // group
    mine = column == row
    qbig[...] = jnp.where(mine, spread, 0.0).astype(jnp.bfloat16)
    earlier = lax.broadcasted_iota(jnp.int32, (CHUNK, CHUNK), 1)
    later = lax.broadcasted_iota(jnp.int32, (CHUNK, CHUNK), 0)
    after = jnp.where(later > earlier, 1.0, 0.0).astype(jnp.bfloat16)

    def deferred(d):
        inner = jnp.logical_and(d > 0, d < count - 1)
        return jnp.logical_and(inner, (d < count // 2) != (me < count // 2))

    def block_copy(d, c):
        here = pl.ds(pl.multiple_of(c * CHUNK, CHUNK), CHUNK)
        there = pl.ds(pl.multiple_of(me * rows + c * CHUNK, CHUNK), CHUNK)
        return pltpu.make_async_remote_copy(
            src_ref=proj.at[d, here, :],
            dst_ref=recv.at[there, :],
            send_sem=send_sem.at[d],
            recv_sem=recv_sem.at[me],
            device_id={"sp": d},
            device_id_type=MESH,
        )

    def step(i, state):
        kept, total = state
        c = chunks - 1 - i
        at = pl.ds(pl.multiple_of(c * CHUNK, CHUNK), CHUNK)
        tok_copy(c).wait()
        for j in range(count):
            d = dest(j)

            @pl.when(i == 0)
            def _():
                w_copy(d).wait()
                if j == 0:
                    for k in range(2, count):
                        w_copy(dest(k)).start()
                    tok_copy(c - 1).start()

            if j == 0:

                @pl.when(i + 2 < chunks)
                def _():
                    tok_copy(c - 2).start()

            block = jnp.dot(
                tok[at, :], wts[d], preferred_element_type=jnp.float32
            ).astype(jnp.bfloat16)
            proj[d, at, :] = block
            if j == count - 1:
                own = pl.ds(pl.multiple_of(me * rows + c * CHUNK, CHUNK), CHUNK)
                recv[own, :] = block
            if j > 0:
                before = dest(j - 1)
                if j == 1:

                    @pl.when(i == 0)
                    def _():
                        pl.semaphore_wait(barrier, count - 1)

                @pl.when(jnp.logical_not(deferred(before)))
                def _():
                    block_copy(before, c).start()

        logits = jnp.zeros((heads, CHUNK), jnp.float32)
        for b in range(half):
            logits = logits + lax.dot_general(
                qbig[:, b * width : (b + 1) * width],
                proj[b, at, :],
                (((1,), (1,)), ((), ())),
                preferred_element_type=jnp.float32,
            )
        logits = logits * HD ** (-0.5) + offsets
        keep = -(jnp.maximum(logits, 0.0) + jnp.log1p(jnp.exp(-jnp.abs(logits))))
        high = keep.astype(jnp.bfloat16)
        rest = keep - high.astype(jnp.float32)
        mid = rest.astype(jnp.bfloat16)
        low = (rest - mid.astype(jnp.float32)).astype(jnp.bfloat16)
        sums = jnp.dot(
            jnp.concatenate([high, mid, low], axis=0), after, preferred_element_type=jnp.float32
        )
        between = sums[:heads] + sums[heads : 2 * heads] + sums[2 * heads :]
        weight = jnp.exp(logits + keep + between + kept)
        weight_high = weight.astype(jnp.bfloat16)
        weight_low = (weight - weight_high.astype(jnp.float32)).astype(jnp.bfloat16)
        both = jnp.concatenate([weight_high, weight_low], axis=0)
        summed = jnp.concatenate(
            [
                jnp.dot(both, proj[half + b, at, :], preferred_element_type=jnp.float32)
                for b in range(half)
            ],
            axis=1,
        )
        total = total + summed[:heads] + summed[heads:]
        kept = kept + jnp.sum(keep, axis=1, keepdims=True)
        return kept, total

    kept, total = lax.fori_loop(
        0,
        chunks,
        step,
        (jnp.zeros((heads, 1), jnp.float32), jnp.zeros((heads, KVH * HD), jnp.float32)),
    )
    total = jnp.where(mine, total, 0.0)
    folded = total[:, :LANES]
    for g in range(1, KVH * HD // LANES):
        folded = folded + total[:, g * LANES : (g + 1) * LANES]
    spread_kept = jnp.broadcast_to(kept, (heads, LANES))
    part[0] = folded
    part[1] = spread_kept
    parts[me, 0] = folded
    parts[me, 1] = spread_kept

    @pl.loop(0, 1)
    def _(i):
        for j in range(count - 1):
            d = dest(j)

            @pl.when(deferred(d))
            def _():
                block_copy(d, chunks - 1 - i).start()

    def part_copy(d):
        return pltpu.make_async_remote_copy(
            src_ref=part,
            dst_ref=parts.at[me],
            send_sem=psend_sem.at[d],
            recv_sem=precv_sem.at[me],
            device_id={"sp": d},
            device_id_type=MESH,
        )

    for j in range(count - 1):
        part_copy(dest(j)).start()

    @pl.loop(1, chunks)
    def _(i):
        for j in range(count - 1):
            d = dest(j)

            @pl.when(deferred(d))
            def _():
                block_copy(d, chunks - 1 - i).start()

    for j in range(count - 1):
        d = dest(j)
        pltpu.make_async_remote_copy(
            src_ref=part,
            dst_ref=parts.at[d],
            send_sem=psend_sem.at[d],
            recv_sem=precv_sem.at[d],
            device_id={"sp": d},
            device_id_type=MESH,
        ).wait()
    left = jnp.zeros((heads, LANES), jnp.float32)
    out = jnp.zeros((heads, LANES), jnp.float32)
    for z in range(count - 1, -1, -1):
        out = out + jnp.exp(left) * parts[z, 0]
        left = left + parts[z, 1]
    turned = pltpu.roll(out, HD, axis=1)
    low_half = lax.broadcasted_iota(jnp.int32, (1, LANES), 1) < HD
    for m in range(heads // 2):
        first, second = 2 * m, 2 * m + 1
        from_first = out if (first // group) % 2 == 0 else turned
        from_second = out if (second // group) % 2 == 1 else turned
        piece = jnp.where(
            low_half, from_first[first : first + 1], from_second[second : second + 1]
        )
        read_ref[:, m * LANES : (m + 1) * LANES] = piece.astype(read_ref.dtype)
    for j in range(count - 1):
        d = dest(j)
        pltpu.make_async_remote_copy(
            src_ref=proj.at[d],
            dst_ref=recv.at[pl.ds(pl.multiple_of(d * rows, CHUNK), rows), :],
            send_sem=send_sem.at[d],
            recv_sem=recv_sem.at[d],
            device_id={"sp": d},
            device_id_type=MESH,
        ).wait()


def place_kernel(count, got, read, cache, read_out, sems):
    rows = got.shape[0] // count
    copies = []
    for k in range(count):
        at = pl.ds(k * rows, rows)
        copies.append(pltpu.make_async_copy(got.at[at, :], cache.at[at, :], sems.at[k]))
    copies.append(pltpu.make_async_copy(read, read_out, sems.at[count]))
    for copy in copies:
        copy.start()
    for copy in copies:
        copy.wait()


def local(tokens, kv_weight, queries, score_offset):
    seq_count, rows, model_width = tokens.shape
    features = kv_weight.shape[1]
    heads = score_offset.shape[0]
    count = lax.axis_size("sp")
    width = features // (count // seq_count)
    fits = (
        seq_count == 1
        and count % 2 == 0
        and count > 2
        and width % LANES == 0
        and rows % CHUNK == 0
        and rows >= 2 * CHUNK
        and features == 2 * KVH * HD
        and 2 * HD == LANES
        and heads % 2 == 0
    )
    if not fits:
        return local_plain(tokens, kv_weight, queries, score_offset)
    length = rows * count
    vmem = pl.BlockSpec(memory_space=pltpu.VMEM)
    hbm = pl.BlockSpec(memory_space=pltpu.HBM)
    got, read = pl.pallas_call(
        functools.partial(exchange_kernel, count),
        out_shape=(
            pltpu.VMEM((length, width), jnp.bfloat16),
            pltpu.VMEM((1, heads * HD), jnp.bfloat16),
        ),
        in_specs=[hbm, hbm, vmem, vmem],
        out_specs=(vmem, vmem),
        scratch_shapes=[
            pltpu.VMEM((rows, model_width), jnp.bfloat16),
            pltpu.VMEM((count, model_width, width), jnp.bfloat16),
            pltpu.VMEM((count, rows, width), jnp.bfloat16),
            pltpu.VMEM((heads, KVH * HD), jnp.bfloat16),
            pltpu.VMEM((2, heads, LANES), jnp.float32),
            pltpu.VMEM((count, 2, heads, LANES), jnp.float32),
            pltpu.SemaphoreType.DMA((rows // CHUNK,)),
            pltpu.SemaphoreType.DMA((count,)),
            pltpu.SemaphoreType.DMA((count,)),
            pltpu.SemaphoreType.DMA((count,)),
            pltpu.SemaphoreType.DMA((count,)),
            pltpu.SemaphoreType.DMA((count,)),
        ],
        compiler_params=pltpu.CompilerParams(
            collective_id=0, has_side_effects=True, vmem_limit_bytes=VMEM_LIMIT
        ),
    )(
        tokens.reshape(rows, model_width),
        kv_weight,
        queries,
        score_offset.reshape(1, heads),
    )
    cache, read = pl.pallas_call(
        functools.partial(place_kernel, count),
        out_shape=(
            jax.ShapeDtypeStruct((length, width), jnp.bfloat16),
            jax.ShapeDtypeStruct((1, heads * HD), jnp.bfloat16),
        ),
        in_specs=[vmem, vmem],
        out_specs=(hbm, hbm),
        scratch_shapes=[pltpu.SemaphoreType.DMA((count + 1,))],
        compiler_params=pltpu.CompilerParams(vmem_limit_bytes=8 * 2**20),
    )(got, read)
    return cache.reshape(1, 1, length, width), read


def solution(mesh):
    placed = (P(("gr", "tp"), "sp", None), P(), P(("gr", "tp"), None), P())
    return jax.shard_map(
        local,
        mesh=mesh,
        in_specs=placed,
        out_specs=(P(("gr", "tp"), "sp", None, None), P(("gr", "tp"), None)),
        check_vma=False,
    )
```

```python
import functools

import jax
import jax.numpy as jnp
from jax import lax
from jax.experimental import pallas as pl
from jax.experimental.pallas import tpu as pltpu
from jax.sharding import PartitionSpec as P

KVH = 8
HD = 64


def prefix(shard, axis, combine, identity):
    size, index = (lax.axis_size(axis), lax.axis_index(axis))
    everything = lax.all_gather(shard, axis)
    start = jnp.broadcast_to(jnp.asarray(identity, shard.dtype), shard.shape)

    def hop(k, before):
        at = size - 1 - k
        reached = at > index
        new = combine(before, everything[at])
        return jnp.where(reached, new, before)

    return lax.fori_loop(0, size, hop, start)


def add_terms(earlier, later):
    return earlier + later


def finish(contribution):
    return lax.psum(contribution, "sp").astype(jnp.bfloat16)


def local_plain(tokens, kv_weight, queries, score_offset):
    seq_count, pos_rows, model_width = tokens.shape
    features = kv_weight.shape[1]
    slot_count = lax.axis_size("sp")
    blocks = slot_count // seq_count
    block_width = features // blocks
    half_blocks = blocks // 2
    heads = score_offset.shape[0]
    group_size = heads // KVH
    per_block = block_width // HD
    projected = jnp.einsum(
        "spd,dcw->scpw",
        tokens,
        kv_weight.reshape(model_width, blocks, block_width),
        preferred_element_type=jnp.float32,
    ).astype(jnp.bfloat16)
    received = lax.all_to_all(
        projected.reshape(slot_count, pos_rows, block_width),
        "sp",
        split_axis=0,
        concat_axis=1,
        tiled=True,
    )
    length = received.shape[1]
    cache = received.reshape(1, 1, length, block_width)
    key_part = projected[:, :half_blocks].reshape(seq_count, half_blocks, pos_rows, per_block, HD)
    value_part = (
        projected[:, half_blocks:]
        .reshape(seq_count, half_blocks, pos_rows, per_block, HD)
        .astype(jnp.float32)
    )
    query_heads = queries.reshape(seq_count, half_blocks, per_block, group_size, HD)
    offsets = score_offset.reshape(half_blocks, per_block, group_size)
    logits = jnp.einsum(
        "scvgd,scpvd->scvgp", query_heads, key_part, preferred_element_type=jnp.float32
    )
    logits = logits * HD ** (-0.5) + offsets[None, :, :, :, None]
    keep_log = jax.nn.log_sigmoid(-logits)
    between = lax.cumsum(keep_log, axis=4, reverse=True) - keep_log
    totals = jnp.sum(keep_log, axis=4)
    later_keep = prefix(totals, "sp", add_terms, jnp.zeros_like(totals))
    weights = jnp.exp(jax.nn.log_sigmoid(logits) + between + later_keep[..., None])
    weighted = jnp.einsum("scvgp,scpvd->scvgd", weights, value_part)
    contribution = weighted.reshape(seq_count, heads * HD)
    return (cache, finish(contribution))


CHUNK = 128
VMEM_LIMIT = 56 * 2**20
LANES = 128
MESH = pl.DeviceIdType.MESH


def exchange_kernel(
    count,
    tok_hbm,
    w_hbm,
    q_ref,
    off_ref,
    recv,
    read_ref,
    tok,
    wts,
    proj,
    qbig,
    part,
    parts,
    tok_sem,
    w_sem,
    send_sem,
    recv_sem,
    psend_sem,
    precv_sem,
):
    me = lax.axis_index("sp")
    rows = tok.shape[0]
    width = wts.shape[2]
    chunks = rows // CHUNK
    heads = off_ref.shape[1]
    group = heads // KVH
    half = count // 2

    lower = me < count // 2

    def dest(j):
        if j == count - 1:
            return me
        down = count - 1 - j
        return jnp.where(
            lower,
            jnp.where(down > me, down, down - 1),
            jnp.where(j < me, j, j + 1),
        )

    def tok_copy(c):
        at = pl.ds(pl.multiple_of(c * CHUNK, CHUNK), CHUNK)
        return pltpu.make_async_copy(tok_hbm.at[at, :], tok.at[at, :], tok_sem.at[c])

    def w_copy(d):
        at = pl.ds(pl.multiple_of(d * width, width), width)
        return pltpu.make_async_copy(w_hbm.at[:, at], wts.at[d], w_sem.at[d])

    barrier = pltpu.get_barrier_semaphore()
    for j in range(count - 1):
        pl.semaphore_signal(barrier, inc=1, device_id={"sp": dest(j)}, device_id_type=MESH)

    tok_copy(chunks - 1).start()
    for j in range(2):
        w_copy(dest(j)).start()

    q_rows = []
    for h in range(heads):
        pair = q_ref[:, h // 2 * LANES : (h // 2 + 1) * LANES].astype(jnp.float32)
        q_rows.append(pair if h % 2 == h // group % 2 else pltpu.roll(pair, HD, axis=1))
    spread = jnp.concatenate(
        [jnp.concatenate(q_rows, axis=0)] * (KVH * HD // LANES), axis=1
    )
    square = (heads, heads)
    diagonal = lax.broadcasted_iota(jnp.int32, square, 0) == lax.broadcasted_iota(
        jnp.int32, square, 1
    )
    offsets = jnp.sum(
        jnp.where(diagonal, jnp.broadcast_to(off_ref[...], square), 0.0), axis=1, keepdims=True
    )
    column = lax.broadcasted_iota(jnp.int32, spread.shape, 1) // HD
    row = lax.broadcasted_iota(jnp.int32, spread.shape, 0) // group
    mine = column == row
    qbig[...] = jnp.where(mine, spread, 0.0).astype(jnp.bfloat16)
    earlier = lax.broadcasted_iota(jnp.int32, (CHUNK, CHUNK), 1)
    later = lax.broadcasted_iota(jnp.int32, (CHUNK, CHUNK), 0)
    after = jnp.where(later > earlier, 1.0, 0.0).astype(jnp.bfloat16)

    def deferred(d):
        inner = jnp.logical_and(d > 0, d < count - 1)
        return jnp.logical_and(inner, (d < count // 2) != (me < count // 2))

    def block_copy(d, c):
        here = pl.ds(pl.multiple_of(c * CHUNK, CHUNK), CHUNK)
        there = pl.ds(pl.multiple_of(me * rows + c * CHUNK, CHUNK), CHUNK)
        return pltpu.make_async_remote_copy(
            src_ref=proj.at[d, here, :],
            dst_ref=recv.at[there, :],
            send_sem=send_sem.at[d],
            recv_sem=recv_sem.at[me],
            device_id={"sp": d},
            device_id_type=MESH,
        )

    def step(i, state):
        kept, total = state
        c = chunks - 1 - i
        at = pl.ds(pl.multiple_of(c * CHUNK, CHUNK), CHUNK)
        tok_copy(c).wait()
        for j in range(count):
            d = dest(j)

            @pl.when(i == 0)
            def _():
                w_copy(d).wait()
                if j == 0:
                    for k in range(2, count):
                        w_copy(dest(k)).start()
                    tok_copy(c - 1).start()

            if j == 0:

                @pl.when(i + 2 < chunks)
                def _():
                    tok_copy(c - 2).start()

            block = jnp.dot(
                tok[at, :], wts[d], preferred_element_type=jnp.float32
            ).astype(jnp.bfloat16)
            proj[d, at, :] = block
            if j == count - 1:
                own = pl.ds(pl.multiple_of(me * rows + c * CHUNK, CHUNK), CHUNK)
                recv[own, :] = block
            if j > 0:
                before = dest(j - 1)
                if j == 1:

                    @pl.when(i == 0)
                    def _():
                        pl.semaphore_wait(barrier, count - 1)

                @pl.when(jnp.logical_not(deferred(before)))
                def _():
                    block_copy(before, c).start()

        logits = jnp.zeros((heads, CHUNK), jnp.float32)
        for b in range(half):
            logits = logits + lax.dot_general(
                qbig[:, b * width : (b + 1) * width],
                proj[b, at, :],
                (((1,), (1,)), ((), ())),
                preferred_element_type=jnp.float32,
            )
        logits = logits * HD ** (-0.5) + offsets
        keep = -(jnp.maximum(logits, 0.0) + jnp.log1p(jnp.exp(-jnp.abs(logits))))
        high = keep.astype(jnp.bfloat16)
        rest = keep - high.astype(jnp.float32)
        mid = rest.astype(jnp.bfloat16)
        low = (rest - mid.astype(jnp.float32)).astype(jnp.bfloat16)
        sums = jnp.dot(
            jnp.concatenate([high, mid, low], axis=0), after, preferred_element_type=jnp.float32
        )
        between = sums[:heads] + sums[heads : 2 * heads] + sums[2 * heads :]
        weight = jnp.exp(logits + keep + between + kept)
        weight_high = weight.astype(jnp.bfloat16)
        weight_low = (weight - weight_high.astype(jnp.float32)).astype(jnp.bfloat16)
        both = jnp.concatenate([weight_high, weight_low], axis=0)
        summed = jnp.concatenate(
            [
                jnp.dot(both, proj[half + b, at, :], preferred_element_type=jnp.float32)
                for b in range(half)
            ],
            axis=1,
        )
        total = total + summed[:heads] + summed[heads:]
        kept = kept + jnp.sum(keep, axis=1, keepdims=True)
        return kept, total

    kept, total = lax.fori_loop(
        0,
        chunks,
        step,
        (jnp.zeros((heads, 1), jnp.float32), jnp.zeros((heads, KVH * HD), jnp.float32)),
    )
    total = jnp.where(mine, total, 0.0)
    folded = total[:, :LANES]
    for g in range(1, KVH * HD // LANES):
        folded = folded + total[:, g * LANES : (g + 1) * LANES]
    spread_kept = jnp.broadcast_to(kept, (heads, LANES))
    part[0] = folded
    part[1] = spread_kept
    parts[me, 0] = folded
    parts[me, 1] = spread_kept

    @pl.loop(0, 1)
    def _(i):
        for j in range(count - 1):
            d = dest(j)

            @pl.when(deferred(d))
            def _():
                block_copy(d, chunks - 1 - i).start()

    def part_copy(d):
        return pltpu.make_async_remote_copy(
            src_ref=part,
            dst_ref=parts.at[me],
            send_sem=psend_sem.at[d],
            recv_sem=precv_sem.at[me],
            device_id={"sp": d},
            device_id_type=MESH,
        )

    for j in range(count - 1):
        part_copy(dest(j)).start()

    @pl.loop(1, chunks)
    def _(i):
        for j in range(count - 1):
            d = dest(j)

            @pl.when(deferred(d))
            def _():
                block_copy(d, chunks - 1 - i).start()

    for j in range(count - 1):
        d = dest(j)
        pltpu.make_async_remote_copy(
            src_ref=part,
            dst_ref=parts.at[d],
            send_sem=psend_sem.at[d],
            recv_sem=precv_sem.at[d],
            device_id={"sp": d},
            device_id_type=MESH,
        ).wait()
    left = jnp.zeros((heads, LANES), jnp.float32)
    out = jnp.zeros((heads, LANES), jnp.float32)
    for z in range(count - 1, -1, -1):
        out = out + jnp.exp(left) * parts[z, 0]
        left = left + parts[z, 1]
    turned = pltpu.roll(out, HD, axis=1)
    low_half = lax.broadcasted_iota(jnp.int32, (1, LANES), 1) < HD
    for m in range(heads // 2):
        first, second = 2 * m, 2 * m + 1
        from_first = out if (first // group) % 2 == 0 else turned
        from_second = out if (second // group) % 2 == 1 else turned
        piece = jnp.where(
            low_half, from_first[first : first + 1], from_second[second : second + 1]
        )
        read_ref[:, m * LANES : (m + 1) * LANES] = piece.astype(read_ref.dtype)
    for j in range(count - 1):
        d = dest(j)
        pltpu.make_async_remote_copy(
            src_ref=proj.at[d],
            dst_ref=recv.at[pl.ds(pl.multiple_of(d * rows, CHUNK), rows), :],
            send_sem=send_sem.at[d],
            recv_sem=recv_sem.at[d],
            device_id={"sp": d},
            device_id_type=MESH,
        ).wait()


def place_kernel(count, got, read, cache, read_out, sems):
    rows = got.shape[0] // count
    copies = []
    for k in range(count):
        at = pl.ds(k * rows, rows)
        copies.append(pltpu.make_async_copy(got.at[at, :], cache.at[at, :], sems.at[k]))
    copies.append(pltpu.make_async_copy(read, read_out, sems.at[count]))
    for k, copy in enumerate(copies):
        copy.start(priority=k % 2)
    for copy in copies:
        copy.wait()


def local(tokens, kv_weight, queries, score_offset):
    seq_count, rows, model_width = tokens.shape
    features = kv_weight.shape[1]
    heads = score_offset.shape[0]
    count = lax.axis_size("sp")
    width = features // (count // seq_count)
    fits = (
        seq_count == 1
        and count % 2 == 0
        and count > 2
        and width % LANES == 0
        and rows % CHUNK == 0
        and rows >= 2 * CHUNK
        and features == 2 * KVH * HD
        and 2 * HD == LANES
        and heads % 2 == 0
    )
    if not fits:
        return local_plain(tokens, kv_weight, queries, score_offset)
    length = rows * count
    vmem = pl.BlockSpec(memory_space=pltpu.VMEM)
    hbm = pl.BlockSpec(memory_space=pltpu.HBM)
    got, read = pl.pallas_call(
        functools.partial(exchange_kernel, count),
        out_shape=(
            pltpu.VMEM((length, width), jnp.bfloat16),
            pltpu.VMEM((1, heads * HD), jnp.bfloat16),
        ),
        in_specs=[hbm, hbm, vmem, vmem],
        out_specs=(vmem, vmem),
        scratch_shapes=[
            pltpu.VMEM((rows, model_width), jnp.bfloat16),
            pltpu.VMEM((count, model_width, width), jnp.bfloat16),
            pltpu.VMEM((count, rows, width), jnp.bfloat16),
            pltpu.VMEM((heads, KVH * HD), jnp.bfloat16),
            pltpu.VMEM((2, heads, LANES), jnp.float32),
            pltpu.VMEM((count, 2, heads, LANES), jnp.float32),
            pltpu.SemaphoreType.DMA((rows // CHUNK,)),
            pltpu.SemaphoreType.DMA((count,)),
            pltpu.SemaphoreType.DMA((count,)),
            pltpu.SemaphoreType.DMA((count,)),
            pltpu.SemaphoreType.DMA((count,)),
            pltpu.SemaphoreType.DMA((count,)),
        ],
        compiler_params=pltpu.CompilerParams(
            collective_id=0, has_side_effects=True, vmem_limit_bytes=VMEM_LIMIT
        ),
    )(
        tokens.reshape(rows, model_width),
        kv_weight,
        queries,
        score_offset.reshape(1, heads),
    )
    cache, read = pl.pallas_call(
        functools.partial(place_kernel, count),
        out_shape=(
            jax.ShapeDtypeStruct((length, width), jnp.bfloat16),
            jax.ShapeDtypeStruct((1, heads * HD), jnp.bfloat16),
        ),
        in_specs=[vmem, vmem],
        out_specs=(hbm, hbm),
        scratch_shapes=[pltpu.SemaphoreType.DMA((count + 1,))],
        compiler_params=pltpu.CompilerParams(vmem_limit_bytes=8 * 2**20),
    )(got, read)
    return cache.reshape(1, 1, length, width), read


def solution(mesh):
    placed = (P(("gr", "tp"), "sp", None), P(), P(("gr", "tp"), None), P())
    return jax.shard_map(
        local,
        mesh=mesh,
        in_specs=placed,
        out_specs=(P(("gr", "tp"), "sp", None, None), P(("gr", "tp"), None)),
        check_vma=False,
    )
```
